32 devices in a mesh: ep: 8 (over z, x), tp: 4 (over y, core).
Axes of the slice: x: 2, y: 2, z: 4, core: 2. Of those that a mesh axis runs over, the one named last changes fastest.
Arguments:
- stream: bfloat16 [128, 4096], P(None, 'ep'), may hold values from -6.5 to 6.5
- norm_gain: float32 [4096], P('ep'), may hold values from 0.1 to 1.9
- w_query: bfloat16 [4096, 2048], P('ep', 'tp'), may hold values from -0.09375 to 0.09375
- w_key: bfloat16 [4096, 1024], P('ep', 'tp'), may hold values from -0.09375 to 0.09375
- w_value: bfloat16 [4096, 1024], P('ep', 'tp'), may hold values from -0.09375 to 0.09375
- break_offset: float32 [16], P('tp'), may hold values from -10 to -2
- cache_keys: bfloat16 [128, 1024, 8, 128], P('ep', None, 'tp'), may hold values from -6 to 6
- cache_values: bfloat16 [128, 1024, 8, 128], P('ep', None, 'tp'), may hold values from -6 to 6
- lengths: int32 [128], P('ep'), may hold values from 128 to 1024
- w_output: bfloat16 [2048, 4096], P('tp', 'ep'), may hold values from -0.125 to 0.125
- head_gain: float32 [2048], P('tp'), may hold values from 0.1 to 1.9
- ffn_gain: float32 [4096], P('ep'), may hold values from 0.1 to 1.9
- route_experts: int32 [128, 2], replicated, may hold values from 0 to 7, all different within a row; in each aligned block of 128 rows (0 to 127, 128 to 255, ...) at most 64 rows name the same one
- route_weights: float32 [128, 2], replicated, may hold values from 0.1 to 1
- expert_gate: bfloat16 [8, 4096, 1024], P('ep', None, 'tp'), may hold values from -0.09375 to 0.09375
- expert_up: bfloat16 [8, 4096, 1024], P('ep', None, 'tp'), may hold values from -0.09375 to 0.09375
- expert_down: bfloat16 [8, 1024, 4096], P('ep', 'tp'), may hold values from -0.1875 to 0.1875
- dense_gate: bfloat16 [4096, 4096], P('ep', 'tp'), may hold values from -0.09375 to 0.09375
- dense_up: bfloat16 [4096, 4096], P('ep', 'tp'), may hold values from -0.09375 to 0.09375
- dense_down: bfloat16 [4096, 4096], P('tp', 'ep'), may hold values from -0.09375 to 0.09375
- mix_gain: float32 [4096], P('ep'), may hold values from 0.1 to 1.9
Outputs:
- mixed_out: bfloat16 [128, 4096], P(None, 'ep')
- key_rows: bfloat16 [128, 1024], P('ep', 'tp')
- value_rows: bfloat16 [128, 1024], P('ep', 'tp')
The draws below stay inside these ranges and needn't reach their ends.
Inputs may be any that keep to these rules, and one draw needn't show every extreme that they name: `route_experts`: in the whole batch no expert is named by more than 64 pairs, a bound that some block reaches; the 2 experts of a token differ.
All inputs are finite; a program needn't handle non-finite values.
Results may differ from the reference program's by a relative error of at most 0.025.
Values may be sent and summed in bfloat16 or wider, within the bound.
A program may use at most 64 MiB of HBM per device.

```python
import math
import jax
import jax.numpy as jnp
import numpy as np
from jax import lax

D = 4096
HEADS = 16
KVH = 8
HD = 128
FF = 1024
FD = 4096
TOP_K = 2
LEN = 1024
SEQS = 128
EXPERTS = 8
CAP = 64
N_TP = 4


def draw_stream(key, part):
    columns = jnp.arange(D, dtype=jnp.float32) / D
    col_scale = 0.6 * jnp.power(3.0, columns)[None, :]
    base_draw = jnp.clip(jax.random.normal(key, (SEQS, D), jnp.float32), -3.3, 3.3)
    values = base_draw * col_scale
    return values.astype(jnp.bfloat16)


def draw_break_offset(key, part):
    centre = -jnp.log(jnp.float32(LEN))
    spread = jax.random.uniform(jax.random.fold_in(key, 7), (HEADS,), jnp.float32, -1.2, 0.8)
    return (centre + spread).astype(jnp.float32)


def plant(drawn, key, low, high):
    dims = drawn.shape
    place = [jax.random.randint(jax.random.fold_in(key, axis), (), 0, dims[axis]) for axis in range(len(dims))]
    drawn = drawn.at[tuple(place)].set(low)
    longest = dims.index(max(dims))
    place[longest] = (place[longest] + 1) % dims[longest]
    return drawn.at[tuple(place)].set(high)


def levels(rng, shape, split, smallest, top_value):
    def one(dim, blocks):
        steps = jax.random.uniform(jax.random.fold_in(jax.random.fold_in(rng, 6), dim), (blocks,), jnp.float32, smallest / len(split), top_value / len(split))
        return jnp.repeat(jnp.exp(steps), shape[dim] // blocks).reshape((-1,) + (1,) * (len(shape) - dim - 1))

    loudness = one(*split[0])
    for cut in split[1:]:
        loudness = loudness * one(*cut)
    return loudness


def assign_block(rng, own, number, rows, count, top, bound, lean):
    sequence = jax.random.permutation(rng, count)
    crowded, ordinary = portions_of(count, rows * top, bound, lean, True), portions_of(count, rows * top, bound, lean, False)
    places = jnp.arange(count)

    def named(tallies, offset_by):
        used = int((tallies > 0).sum())
        fixed = max(1, used // 4)
        moved = fixed + (places - fixed + offset_by * (used - fixed)) % max(1, count - fixed)
        return jnp.zeros((count,), jnp.int32).at[sequence[jnp.where(places < fixed, places, moved)]].set(jnp.asarray(tallies, jnp.int32))

    tallies = jnp.where(number % 4 == 0, named(crowded, number // 4), named(ordinary, number - number // 4 - 1))
    mixed = jax.random.permutation(jax.random.fold_in(own, 3), count)
    donor, sink = mixed[0:count // 2 * 2:2], mixed[1:count // 2 * 2:2]
    margin = jnp.minimum(tallies[donor] - 1, bound - tallies[sink]) // 2
    margin = jnp.where((donor == sequence[0]) | (sink == sequence[0]) | (tallies[sink] == 0), 0, jnp.maximum(margin, 0))
    moved = jax.random.randint(jax.random.fold_in(own, 4), (count // 2,), 0, 1 << 20) % (margin + 1)
    tallies = tallies.at[donor].add(-moved).at[sink].add(moved)
    members = jnp.searchsorted(jnp.cumsum(tallies), jnp.arange(rows * top), side="right").astype(jnp.int32)
    listing = members.reshape(top, rows).T
    listing = listing[jax.random.permutation(jax.random.fold_in(own, 1), rows)]
    offset_by = jax.random.randint(jax.random.fold_in(own, 2), (rows, 1), 0, top)
    return jnp.take_along_axis(listing, (jnp.arange(top)[None, :] + offset_by) % top, axis=1)


def portions_of(count, total, most, lean, full):
    portions = [(1 << 20) // math.isqrt(rank ** lean) + 1 for rank in range(1, count + 1)]
    largest = most if full else min(most, max(-(-total // count), total * portions[0] // sum(portions)))
    least = 1 if total - largest >= count - 1 else 0
    given, rest = [largest] + [least] * (count - 1), total - largest - least * (count - 1)
    while rest > 0:
        movable = [i for i in range(1, count) if given[i] < largest] or [i for i in range(1, count) if given[i] < most]
        pool, budget = sum([portions[i] for i in movable]), rest
        for i in movable:
            addition = min(most - given[i], max(1, budget * portions[i] // pool), rest)
            given[i] = given[i] + addition
            rest = rest - addition
    return np.array(given)


def normal_values(stream_key, extent, deviation, limit, pieces=(), kind=jnp.bfloat16):
    array = jax.random.normal(stream_key, extent, jnp.float32) * deviation
    if len(pieces) > 0:
        array = levels(stream_key, extent, pieces, -0.22, 0.18) * array
    return jnp.clip(array, min=-limit, max=limit).astype(kind)


def setup_inputs(seed: int = 0) -> dict:
    arg_keys = jax.random.split(jax.random.key(seed), 22)
    stream = draw_stream(jax.random.fold_in(arg_keys[21], 71), 0)
    norm_gain = jnp.clip(1.0 + 0.18 * jax.random.normal(arg_keys[1], (D,), jnp.float32), 0.1, 1.9)
    w_query = normal_values(arg_keys[2], (D, HEADS * HD), D ** -0.5, 0.09375, ((0, 8), (1, 4)))
    w_key = normal_values(arg_keys[3], (D, KVH * HD), D ** -0.5, 0.09375, ((0, 8), (1, 4)))
    w_value = normal_values(arg_keys[4], (D, KVH * HD), D ** -0.5, 0.09375, ((0, 8), (1, 4)))
    break_offset = draw_break_offset(jax.random.fold_in(arg_keys[21], 71), 0)
    cache_keys = normal_values(arg_keys[6], (SEQS, LEN, KVH, HD), 1.0, 6.0, ((0, 8), (2, 4)))
    cache_values = normal_values(arg_keys[7], (SEQS, LEN, KVH, HD), 1.0, 6.0, ((0, 8), (2, 4)))
    lengths = plant(jax.random.randint(arg_keys[8], (SEQS,), LEN // 8, LEN + 1), jax.random.fold_in(arg_keys[8], 1), LEN // 8, LEN).astype(jnp.int32)
    w_output = normal_values(arg_keys[9], (HEADS * HD, D), (HEADS * HD) ** -0.5, 0.125, ((0, 4), (1, 8)))
    head_gain = jnp.clip(1.0 + 0.18 * jax.random.normal(arg_keys[10], (HEADS * HD,), jnp.float32), 0.1, 1.9)
    ffn_gain = jnp.clip(1.0 + 0.18 * jax.random.normal(arg_keys[11], (D,), jnp.float32), 0.1, 1.9)
    route_experts_keys = jax.random.split(jax.random.fold_in(arg_keys[12], 1), SEQS // SEQS)
    route_experts_turns = jax.random.permutation(jax.random.fold_in(arg_keys[12], 3), SEQS // SEQS)
    route_experts = jax.vmap(lambda own, number: assign_block(jax.random.fold_in(arg_keys[12], 2), own, number, SEQS, EXPERTS, TOP_K, CAP, 2))(route_experts_keys, route_experts_turns).reshape((SEQS, TOP_K))
    route_weights = jnp.clip(jax.random.uniform(arg_keys[13], (SEQS, TOP_K), jnp.float32, 0.1, 1.0), 0.1, 1.0)
    expert_gate = normal_values(arg_keys[14], (EXPERTS, D, FF), D ** -0.5, 0.09375, ((0, 8), (2, 4)))
    expert_up = normal_values(arg_keys[15], (EXPERTS, D, FF), D ** -0.5, 0.09375, ((0, 8), (2, 4)))
    expert_down = normal_values(arg_keys[16], (EXPERTS, FF, D), FF ** -0.5, 0.1875, ((0, 8), (1, 4)))
    dense_gate = normal_values(arg_keys[17], (D, FD), D ** -0.5, 0.09375, ((0, 8), (1, 4)))
    dense_up = normal_values(arg_keys[18], (D, FD), D ** -0.5, 0.09375, ((0, 8), (1, 4)))
    dense_down = normal_values(arg_keys[19], (FD, D), FD ** -0.5, 0.09375, ((0, 4), (1, 8)))
    mix_gain = jnp.clip(1.0 + 0.18 * jax.random.normal(arg_keys[20], (D,), jnp.float32), 0.1, 1.9)
    return {"stream": stream, "norm_gain": norm_gain, "w_query": w_query, "w_key": w_key, "w_value": w_value, "break_offset": break_offset, "cache_keys": cache_keys, "cache_values": cache_values, "lengths": lengths, "w_output": w_output, "head_gain": head_gain, "ffn_gain": ffn_gain, "route_experts": route_experts, "route_weights": route_weights, "expert_gate": expert_gate, "expert_up": expert_up, "expert_down": expert_down, "dense_gate": dense_gate, "dense_up": dense_up, "dense_down": dense_down, "mix_gain": mix_gain}


EPSILON = 1e-06

def rms_rows(values, gain_vec):
    return values * lax.rsqrt(lax.optimization_barrier(jnp.mean(values * values, axis=1, keepdims=True)) + EPSILON) * gain_vec[None, :]

def narrow_sum(left_side, right_side):
    per_group = right_side.shape[0] // N_TP
    summed = jnp.zeros((left_side.shape[0], right_side.shape[1]), jnp.float32)
    for group_index in range(N_TP):
        partial_value = jnp.dot(left_side[:, group_index * per_group:(group_index + 1) * per_group], right_side[group_index * per_group:(group_index + 1) * per_group], preferred_element_type=jnp.float32)
        rounded = lax.optimization_barrier(partial_value.astype(jnp.bfloat16))
        summed = summed + rounded.astype(jnp.float32)
    return summed.astype(jnp.bfloat16)

def slot_table(route_experts, experts, capacity):
    chosen = route_experts.reshape(-1)
    onehot = (chosen[:, None] == jnp.arange(experts, dtype=jnp.int32)[None, :]).astype(jnp.int32)
    earlier = jnp.cumsum(onehot, axis=0) - onehot
    rank_in = lax.optimization_barrier(jnp.sum(earlier * onehot, axis=1)).astype(jnp.int32)
    slot_ids = (chosen * capacity + rank_in).astype(jnp.int32)
    owners = jnp.arange(chosen.shape[0], dtype=jnp.int32) // route_experts.shape[1]
    filled = jnp.full((experts * capacity,), route_experts.shape[0], jnp.int32).at[slot_ids].set(owners)
    return (slot_ids, filled)

def reference(stream, norm_gain, w_query, w_key, w_value, break_offset, cache_keys, cache_values, lengths, w_output, head_gain, ffn_gain, route_experts, route_weights, expert_gate, expert_up, expert_down, dense_gate, dense_up, dense_down, mix_gain):
    streamf = stream.astype(jnp.float32)
    normed = rms_rows(streamf, norm_gain).astype(jnp.bfloat16)
    queries = jnp.dot(normed, w_query, preferred_element_type=jnp.float32).astype(jnp.bfloat16)
    key_rows = jnp.dot(normed, w_key, preferred_element_type=jnp.float32).astype(jnp.bfloat16)
    value_rows = jnp.dot(normed, w_value, preferred_element_type=jnp.float32).astype(jnp.bfloat16)
    seq_total = stream.shape[0]
    heads = break_offset.shape[0]
    kv_heads = cache_keys.shape[2]
    head_dim = cache_keys.shape[3]
    group_size = heads // kv_heads
    offsets = break_offset.reshape(kv_heads, group_size)[:, :, None]
    gains = head_gain.reshape(kv_heads, group_size, head_dim)

    def attend(inputs):
        query_one, keys_one, values_one, length_one = inputs
        scores = jnp.einsum('kgd,lkd->kgl', query_one.astype(jnp.float32), keys_one.astype(jnp.float32))
        scores = scores * head_dim ** (-0.5) + offsets
        in_cache = (jnp.arange(keys_one.shape[0], dtype=jnp.int32) < length_one)[None, None, :]
        failed = jnp.where(in_cache, jax.nn.log_sigmoid(-scores), 0.0)
        later_sum = lax.cumsum(failed, axis=2, reverse=True) - failed
        weights = jnp.where(in_cache, jnp.exp(jax.nn.log_sigmoid(scores) + later_sum), 0.0).astype(jnp.bfloat16)
        attended = jnp.einsum('kgl,lkd->kgd', weights.astype(jnp.float32), values_one.astype(jnp.float32))
        normalized = attended * lax.rsqrt(lax.optimization_barrier(jnp.mean(attended * attended, axis=2, keepdims=True)) + EPSILON) * gains
        return normalized.astype(jnp.bfloat16).reshape(heads * head_dim)
    head_out = lax.map(attend, (queries.reshape(seq_total, kv_heads, group_size, head_dim), cache_keys, cache_values, lengths))
    attn_out = narrow_sum(head_out, w_output)
    residual = streamf + attn_out.astype(jnp.float32)
    normed_ffn = rms_rows(residual, ffn_gain).astype(jnp.bfloat16)
    gate_part = jnp.dot(normed_ffn, dense_gate, preferred_element_type=jnp.float32)
    up_part = jnp.dot(normed_ffn, dense_up, preferred_element_type=jnp.float32)
    dense_hidden = (jax.nn.silu(gate_part) * up_part).astype(jnp.bfloat16)
    dense_out = narrow_sum(dense_hidden, dense_down)
    experts = expert_gate.shape[0]
    slot_ids, filled = slot_table(route_experts, experts, CAP)
    padded = jnp.concatenate([normed_ffn, jnp.zeros((1, normed_ffn.shape[1]), jnp.bfloat16)], axis=0)
    expert_in = padded[filled].reshape(experts, CAP, normed_ffn.shape[1])

    def expert_one(inputs):
        rows_in, gate_one, up_one, down_one = inputs
        gate_val = jnp.dot(rows_in, gate_one, preferred_element_type=jnp.float32)
        up_val = jnp.dot(rows_in, up_one, preferred_element_type=jnp.float32)
        expert_hidden = (jax.nn.silu(gate_val) * up_val).astype(jnp.bfloat16)
        return narrow_sum(expert_hidden, down_one)
    expert_out = lax.map(expert_one, (expert_in, expert_gate, expert_up, expert_down))
    picked = expert_out.reshape(experts * CAP, -1)[slot_ids].reshape(seq_total, route_experts.shape[1], -1)
    shares = route_weights / lax.optimization_barrier(jnp.sum(route_weights, axis=1, keepdims=True))
    moe_out = lax.optimization_barrier(jnp.sum(picked.astype(jnp.float32) * shares[:, :, None], axis=1))
    mixed_out = (residual + moe_out + mix_gain[None, :] * dense_out.astype(jnp.float32)).astype(jnp.bfloat16)
    return (mixed_out, key_rows, value_rows)
```

```python
import functools

import jax
import jax.numpy as jnp
from jax import lax
from jax.experimental import pallas as pl
from jax.experimental.pallas import tpu as pltpu
from jax.sharding import PartitionSpec as P

EPSILON = 1e-06
MESH = pl.DeviceIdType.MESH
F32 = jnp.float32
BF16 = jnp.bfloat16
LIMIT_MIB = 48
NT = (((1,), (1,)), ((), ()))


def row_sums(squares):
    ones = jnp.ones((8, squares.shape[1]), BF16)
    high = squares.astype(BF16)
    low = (squares - high.astype(F32)).astype(BF16)
    return lax.dot_general(ones, high, NT, preferred_element_type=F32) + lax.dot_general(
        ones, low, NT, preferred_element_type=F32
    )


def own_column(sums, first, rows):
    width = sums.shape[1]
    lane = lax.broadcasted_iota(jnp.int32, (rows, width), 1)
    row = lax.broadcasted_iota(jnp.int32, (rows, width), 0)
    return jnp.sum(jnp.where(lane == row + first, sums[0:1, :], 0.0), axis=1, keepdims=True)


def plan(n):
    inner = 1 << ((n.bit_length() - 1) // 2)
    return n // inner, inner


def spread(count):
    return sorted(range(1, count), key=lambda d: abs(2 * d - count))


class Grid:
    def __init__(self, n):
        self.nz, self.nx = plan(n)
        self.me = lax.axis_index("ep")
        self.z = self.me // self.nx
        self.x = lax.rem(self.me, self.nx)

    def at(self, dz, dx):
        return lax.rem(self.z + dz, self.nz) * self.nx + lax.rem(self.x + dx, self.nx)

    def source(self, dz, dx):
        return self.at(self.nz - dz, self.nx - dx)

    def peers(self):
        order = spread(self.nz)
        return [(dz, dx) for dz in order for dx in range(self.nx)] + [
            (0, dx) for dx in range(1, self.nx)
        ]


def signal_all(axes):
    barrier = pltpu.get_barrier_semaphore()
    total = 0
    for axis, count in axes:
        me = lax.axis_index(axis)
        for k in range(1, count):
            pl.semaphore_signal(
                barrier, inc=1, device_id={axis: lax.rem(me + k, count)}, device_id_type=MESH
            )
            total += 1
    return barrier, total


def push(axis, peer, src, dst, sems, i):
    copy = pltpu.make_async_remote_copy(
        src_ref=src,
        dst_ref=dst,
        send_sem=sems[0].at[i],
        recv_sem=sems[1].at[i],
        device_id={axis: peer},
        device_id_type=MESH,
    )
    copy.start()
    return copy


def scatter_first(g, part, got, sems):
    copies = {}
    for dz in spread(g.nz) + [0]:
        for dx in range(1, g.nx):
            i = dz * (g.nx - 1) + dx - 1
            copies[dz, dx] = push("ep", g.at(0, dx), part.at[g.at(dz, dx)], got.at[i], sems, i)
    return copies


def scatter_next(g, part, got, copies, mid, got2, sems, dz):
    acc = part[g.at(dz, 0)].astype(F32)
    for dx in range(1, g.nx):
        copies[dz, dx].wait_recv()
        acc = acc + got[dz * (g.nx - 1) + dx - 1].astype(F32)
    if dz == 0:
        return acc
    mid[dz - 1] = acc.astype(BF16)
    return push("ep", g.at(dz, 0), mid.at[dz - 1], got2.at[dz - 1], sems, dz - 1)


def tp_sum(nt, part, arrived, pair, crossed, full, sems, extra):
    me = lax.axis_index("tp")
    core = lax.rem(me, 2)
    partner = me + 1 - 2 * core
    half = pair.shape[0]
    mine = pl.ds(pl.multiple_of(core * half, half), half)
    other = pl.ds(pl.multiple_of((1 - core) * half, half), half)
    copies = [push("tp", partner, part.at[other], arrived, sems, 0)]
    copies[0].wait_recv()
    pair[...] = (part[mine].astype(F32) + arrived[...].astype(F32)).astype(BF16)
    for j in range(1, nt // 2):
        copies.append(push("tp", lax.rem(me + 2 * j, nt), pair, crossed.at[j - 1], sems, j))
    total = pair[...].astype(F32)
    for j in range(1, nt // 2):
        copies[j].wait_recv()
        total = total + crossed[j - 1].astype(F32)
    if extra is not None:
        total = total + extra[mine]
    full[mine] = total.astype(BF16)
    copies.append(push("tp", partner, full.at[mine], full.at[mine], sems, nt // 2))
    copies[-1].wait_recv()
    return copies


def attend(kv, per, waits, len_ref, off_ref, gain_ref, q_s, k_s, v_s, sc_s, sg_s, hl_s, sm_s,
           ho_s):
    heads, rows, hd = q_s.shape
    cols = k_s.shape[1]
    group = heads // kv
    m = per * heads
    lanes = 128
    blocks = cols // lanes
    pairs = rows // per
    row_q = lax.broadcasted_iota(jnp.int32, (m, hd), 0)
    row = lax.broadcasted_iota(jnp.int32, (m, lanes), 0)
    lane = lax.broadcasted_iota(jnp.int32, (m, lanes), 1)
    for p in range(pairs):
        q = jnp.concatenate(
            [q_s[h, pl.ds(p * per + s, 1), :] for s in range(per) for h in range(heads)], axis=0
        )
        wide = jnp.concatenate(
            [jnp.where(row_q // heads == s, q, 0.0) for s in range(per)], axis=1
        ).astype(BF16)
        waits[0][p].wait()
        keys = jnp.concatenate([k_s[p * per + s] for s in range(per)], axis=1)
        sc_s[p] = lax.dot_general(wide, keys, NT, preferred_element_type=F32)
    offset = jnp.zeros((m, lanes), F32)
    for h in range(heads):
        offset = jnp.where(row % heads == h, off_ref[h], offset)
    mine = (row % heads) // group == lane % kv
    limits = []
    for p in range(pairs):
        length = jnp.zeros((m, lanes), jnp.int32)
        for s in range(per):
            length = jnp.where(row // heads == s, len_ref[p * per + s], length)
        limit = jnp.where(mine, length * kv - lane, -cols)
        limits.append(limit)
        fails = []
        for b in range(blocks):
            sc = sc_s[p, :, b * lanes : (b + 1) * lanes] * hd ** (-0.5) + offset
            ls = jnp.minimum(sc, 0.0) - jnp.log(1.0 + jnp.exp(-jnp.abs(sc)))
            sg_s[p, :, b * lanes : (b + 1) * lanes] = ls
            fails.append(jnp.where(limit > b * lanes, ls - sc, 0.0))
        failed = jnp.concatenate(fails, axis=0)
        high = failed.astype(BF16)
        low = (failed - high.astype(F32)).astype(BF16)
        hl_s[p] = jnp.concatenate([high, low], axis=1)
    r = lax.broadcasted_iota(jnp.int32, (2 * lanes, 2 * lanes), 0) % lanes
    c = lax.broadcasted_iota(jnp.int32, (2 * lanes, 2 * lanes), 1)
    tri = jnp.where((r > c) | (c >= lanes), 1.0, 0.0).astype(BF16)
    for p in range(pairs):
        sm_s[p] = jnp.dot(hl_s[p], tri, preferred_element_type=F32)
    gains = jnp.concatenate([gain_ref[...]] * per, axis=0)
    for p in range(pairs):
        acc = jnp.zeros((m, lanes), F32)
        weights = [None] * blocks
        for b in reversed(range(blocks)):
            later = sm_s[p, b * m : (b + 1) * m, :lanes] + acc
            acc = acc + sm_s[p, b * m : (b + 1) * m, lanes:]
            weights[b] = jnp.where(
                limits[p] > b * lanes,
                jnp.exp(sg_s[p, :, b * lanes : (b + 1) * lanes] + later),
                0.0,
            )
        weights = jnp.concatenate(weights, axis=1).astype(BF16)
        waits[1][p].wait()
        values = jnp.concatenate([v_s[p * per + s] for s in range(per)], axis=1)
        both = jnp.dot(weights, values, preferred_element_type=F32)
        att = both[:, :hd]
        for s in range(1, per):
            att = jnp.where(row_q // heads == s, both[:, s * hd : (s + 1) * hd], att)
        att = att * lax.rsqrt(jnp.mean(att * att, axis=1, keepdims=True) + EPSILON) * gains
        for s in range(per):
            for h in range(heads):
                ho_s[h, pl.ds(p * per + s, 1), :] = att[s * heads + h : s * heads + h + 1]


def layer_kernel(
    n, nt, kv, per, width, cap,
    x_hbm, g_hbm, wq_hbm, wk_hbm, wv_hbm,
    len_hbm, off_hbm, gain_hbm, fg_hbm, mix_hbm, route_hbm, route_w_hbm,
    key_hbm, val_hbm, wo_hbm, dg_hbm, du_hbm, dd_hbm, eg_hbm, eu_hbm, ed_hbm,
    out_ref, k_ref, v_ref,
    x_ref, g_ref, wq_ref, wk_ref, wv_ref,
    len_ref, off_ref, gain_ref, fg_ref, mix_ref, route_ref, route_w_ref, e_sem,
    k_s, v_s, wo, dg, du, dd, eg, eu, ed, k_sem, v_sem, w_sem,
    p_part, p_got, p_mid, p_got2, p_sums, p_sums_in,
    q_s, sc_s, sg_s, hl_s, sm_s, ho_s,
    heads_all, part, part2, disp, disp_in, sums, sums_in,
    gu, gu_got, gu_mid, gu_got2, hid_all, act_s, share_s,
    ret_x, ret_p, ret, ret_in, res,
    a_in, a_pair, a_cross, a_full, f_in, f_pair, f_cross, f_full,
    *sem_refs,
):
    (p1, p2, ps, hs, ds, ws, ss, g1, g2, i1, i2, rs, as_, fs, xs) = [
        (sem_refs[2 * i], sem_refs[2 * i + 1]) for i in range(len(sem_refs) // 2)
    ]
    g = Grid(n)
    me = g.me
    barrier, greetings = signal_all((("ep", n), ("tp", nt)))
    early = [
        pltpu.make_async_copy(src, dst, e_sem.at[i])
        for i, (src, dst) in enumerate(
            ((x_hbm, x_ref), (g_hbm, g_ref), (wq_hbm, wq_ref), (wk_hbm, wk_ref),
             (wv_hbm, wv_ref), (len_hbm, len_ref), (off_hbm, off_ref), (gain_hbm, gain_ref),
             (fg_hbm, fg_ref), (mix_hbm, mix_ref), (route_hbm, route_ref),
             (route_w_hbm, route_w_ref))
        )
    ]
    for load in early:
        load.start()
    pairs = k_s.shape[0] // per
    k_loads, v_loads = [], []
    for p in range(pairs):
        rng = pl.ds(p * per, per)
        k_loads.append(pltpu.make_async_copy(key_hbm.at[rng], k_s.at[rng], k_sem.at[p]))
        v_loads.append(pltpu.make_async_copy(val_hbm.at[rng], v_s.at[rng], v_sem.at[p]))
    loads = [
        pltpu.make_async_copy(src, dst, w_sem.at[i])
        for i, (src, dst) in enumerate(
            ((wo_hbm, wo), (dg_hbm, dg), (du_hbm, du), (eg_hbm.at[0], eg), (eu_hbm.at[0], eu),
             (ed_hbm.at[0], ed), (dd_hbm, dd))
        )
    ]
    total_rows, block = x_ref.shape
    rows = total_rows // n
    sent = []

    for load in early:
        load.wait()
    for load in k_loads + v_loads + loads:
        load.start()
    x = x_ref[...].astype(F32)
    xg = (x * g_ref[...]).astype(BF16)
    p_sums[...] = row_sums(x * x)
    at = 0
    for w_ref in (wq_ref, wk_ref, wv_ref):
        cols = w_ref.shape[1]
        val = jnp.dot(xg, w_ref[...], preferred_element_type=F32).astype(BF16)
        for i in range(n):
            p_part[i, :, at : at + cols] = val[i * rows : (i + 1) * rows]
        at += cols
    pl.semaphore_wait(barrier, greetings)
    first = scatter_first(g, p_part, p_got, p1)
    p_s = {
        (dz, dx): push("ep", g.at(dz, dx), p_sums.at[pl.ds(0, 1)],
                       p_sums_in.at[dz * g.nx + dx - 1], ps, dz * g.nx + dx - 1)
        for dz, dx in g.peers()
    }
    second = {}
    for dz in spread(g.nz) + [0]:
        second[dz] = scatter_next(g, p_part, p_got, first, p_mid, p_got2, p2, dz)
    total = second.pop(0)
    squares = p_sums[0:1, :]
    for dz, dx in g.peers():
        p_s[dz, dx].wait_recv()
        squares = squares + p_sums_in[dz * g.nx + dx - 1]
    mean = own_column(squares, me * rows, rows) / width
    for dz in second:
        second[dz].wait_recv()
        total = total + p_got2[dz - 1].astype(F32)
    sent += list(first.values()) + list(p_s.values()) + list(second.values())
    total = total * lax.rsqrt(mean + EPSILON)
    hd = q_s.shape[2]
    q_width = wq_ref.shape[1]
    k_width = wk_ref.shape[1]
    for h in range(q_s.shape[0]):
        q_s[h] = total[:, h * hd : (h + 1) * hd].astype(BF16).astype(F32)
    k_ref[...] = total[:, q_width : q_width + k_width].astype(BF16)
    v_ref[...] = total[:, q_width + k_width :].astype(BF16)

    attend(kv, per, (k_loads, v_loads), len_ref, off_ref, gain_ref, q_s, k_s, v_s, sc_s, sg_s,
           hl_s, sm_s, ho_s)
    heads_all[me] = jnp.concatenate(
        [ho_s[h] for h in range(ho_s.shape[0])], axis=1
    ).astype(BF16)
    copies = [
        push("ep", g.at(dz, dx), heads_all.at[me], heads_all.at[me], hs, dz * g.nx + dx - 1)
        for dz, dx in g.peers()
    ]
    sent += copies
    me_t = lax.axis_index("tp")
    core = lax.rem(me_t, 2)
    partner = me_t + 1 - 2 * core
    half = cap // 2
    near = pl.ds(pl.multiple_of(core * half, half), half)
    far = pl.ds(pl.multiple_of((1 - core) * half, half), half)
    top = route_ref.shape[0]
    expert_ids = lax.broadcasted_iota(jnp.int32, (n, total_rows), 0)
    named = [
        jnp.where(route_ref[k : k + 1, :] == expert_ids, 1.0, 0.0).astype(F32)
        for k in range(top)
    ]
    token_r = lax.broadcasted_iota(jnp.int32, (total_rows, total_rows), 0)
    token_c = lax.broadcasted_iota(jnp.int32, (total_rows, total_rows), 1)
    before = jnp.dot(
        sum(named).astype(BF16),
        jnp.where(token_r < token_c, 1.0, 0.0).astype(BF16),
        preferred_element_type=F32,
    )
    slots = [
        jnp.sum(named[k] * before, axis=0, keepdims=True)
        + route_ref[k : k + 1, :].astype(F32) * cap
        for k in range(top)
    ]
    columns = [
        jnp.sum(jnp.where(token_r == token_c, slot, 0.0), axis=1, keepdims=True)
        for slot in slots
    ]
    share_sum = route_w_ref[0:1, :]
    for k in range(1, top):
        share_sum = share_sum + route_w_ref[k : k + 1, :]
    share_rows = [route_w_ref[k : k + 1, :] / share_sum for k in range(top)]
    slot_rows = lax.broadcasted_iota(jnp.int32, (cap, total_rows), 0)
    half_rows = lax.broadcasted_iota(jnp.int32, (half, total_rows), 0) + core * half

    def picks(expert, places):
        place = (places + expert * cap).astype(F32)
        return [slot == place for slot in slots]

    peers = g.peers()
    mine = picks(me, slot_rows)
    hit = functools.reduce(jnp.logical_or, mine)
    chosen = jnp.concatenate(
        [
            jnp.where(functools.reduce(jnp.logical_or, picks(g.at(dz, dx), half_rows)), 1.0, 0.0)
            for dz, dx in peers
        ]
        + [jnp.where(hit, 1.0, 0.0)],
        axis=0,
    ).astype(BF16)
    slot_cols = lax.broadcasted_iota(jnp.int32, (total_rows, half), 1) + core * half

    def returns(expert):
        place = (slot_cols + expert * cap).astype(F32)
        hits = functools.reduce(jnp.logical_or, [column == place for column in columns])
        return jnp.where(hits, 1.0, 0.0).astype(BF16)

    loads[0].wait()
    for copy in copies:
        copy.wait_recv()
    all_heads = heads_all[...].reshape(total_rows, heads_all.shape[2])
    part[...] = jnp.dot(all_heads, wo[...], preferred_element_type=F32).astype(BF16)
    sent += tp_sum(nt, part, a_in, a_pair, a_cross, a_full, as_, None)
    residual = x_ref[...].astype(F32) + a_full[...].astype(F32)
    u = (residual * fg_ref[...]).astype(BF16)
    sums[...] = row_sums(residual * residual)
    res[...] = residual
    packed = jnp.dot(chosen, u, preferred_element_type=F32).astype(BF16)
    d_copies, s_copies = {}, {}
    for j, (dz, dx) in enumerate(peers):
        i = dz * g.nx + dx - 1
        disp[i] = packed[j * half : (j + 1) * half]
        d_copies[i] = push("ep", g.at(dz, dx), disp.at[i], disp_in.at[i, near], ds, i)
    for dz, dx in peers:
        i = dz * g.nx + dx - 1
        s_copies[i] = push("ep", g.at(dz, dx), sums.at[pl.ds(0, 1)], sums_in.at[i], ss, i)
    sent += list(d_copies.values()) + list(s_copies.values())
    own_in = packed[len(peers) * half :]
    hidden = dg.shape[1]
    for load, w, at in ((loads[1], dg, 0), (loads[2], du, hidden)):
        load.wait()
        val = jnp.dot(u, w[...], preferred_element_type=F32).astype(BF16)
        for i in range(n):
            gu[i, :, at : at + hidden] = val[i * rows : (i + 1) * rows]
    g_first = scatter_first(g, gu, gu_got, g1)
    loads[3].wait()
    loads[4].wait()
    span = pl.ds(pl.multiple_of(me * block, block), block)
    gate = jnp.dot(own_in, eg[span, :], preferred_element_type=F32)
    up = jnp.dot(own_in, eu[span, :], preferred_element_type=F32)
    squares = sums[0:1, :]
    order = list(reversed(peers))
    g_order = spread(g.nz) + [0]
    g_second = {}
    forwards = {}
    lead = max(1, len(order) - len(g_order))
    for j in range(len(order) + 1):
        if j < len(order):
            dz, dx = order[j]
            i = dz * g.nx + dx - 1
            d_copies[i].wait_recv()
            forwards[i] = push("tp", partner, disp_in.at[i, near], disp_in.at[i, near], ws, i)
        if 0 <= j - lead < len(g_order):
            dz = g_order[j - lead]
            g_second[dz] = scatter_next(g, gu, gu_got, g_first, gu_mid, gu_got2, g2, dz)
        if j > 0:
            dz, dx = order[j - 1]
            i = dz * g.nx + dx - 1
            s_copies[i].wait_recv()
            squares = squares + sums_in[i]
            forwards[i].wait_recv()
            span = pl.ds(pl.multiple_of(g.source(dz, dx) * block, block), block)
            gate = gate + jnp.dot(disp_in[i], eg[span, :], preferred_element_type=F32)
            up = up + jnp.dot(disp_in[i], eu[span, :], preferred_element_type=F32)
    for dz in g_order:
        if dz not in g_second:
            g_second[dz] = scatter_next(g, gu, gu_got, g_first, gu_mid, gu_got2, g2, dz)
    gate_up = g_second.pop(0)
    sent += list(forwards.values()) + list(g_first.values()) + list(g_second.values())
    scale_row = lax.rsqrt(squares / width + EPSILON)
    scale = jnp.sum(jnp.where(hit, scale_row, 0.0), axis=1, keepdims=True)
    share = jnp.zeros((cap, 1), F32)
    for k in range(len(mine)):
        share = share + jnp.sum(
            jnp.where(mine[k], share_rows[k], 0.0), axis=1, keepdims=True
        )
    gate = gate * scale
    up = up * scale
    act_s[...] = (gate / (1.0 + jnp.exp(-gate)) * up).astype(BF16)
    share_s[...] = jnp.broadcast_to(share, share_s.shape)
    loads[5].wait()
    out = jnp.dot(act_s[far], ed[...], preferred_element_type=F32) * share_s[far][:, 0:1]
    for i in range(n):
        ret_x[i] = out[:, i * block : (i + 1) * block].astype(BF16)
    swap = push("tp", partner, ret_x, ret_p, xs, 0)
    sent.append(swap)
    out = jnp.dot(act_s[near], ed[...], preferred_element_type=F32) * share_s[near][:, 0:1]
    for i in range(n):
        ret[i] = out[:, i * block : (i + 1) * block]
    swap.wait_recv()
    for i in range(n):
        ret_x2 = ret[i] + ret_p[i].astype(F32)
        ret_p[i] = ret_x2.astype(BF16)
    r_copies = {}
    for dz, dx in peers:
        i = dz * g.nx + dx - 1
        r_copies[i] = push("ep", g.at(dz, dx), ret_p.at[g.at(dz, dx)], ret_in.at[i + 1], rs, i)
    sent += list(r_copies.values())
    ret_in[0] = ret_p[me]
    for dz in g_second:
        g_second[dz].wait_recv()
        gate_up = gate_up + gu_got2[dz - 1].astype(F32)
    gate_up = gate_up * own_column(scale_row, me * rows, rows)
    dense_gate = gate_up[:, :hidden]
    hid_all[me] = (dense_gate / (1.0 + jnp.exp(-dense_gate)) * gate_up[:, hidden:]).astype(BF16)
    i_first = {
        dz: push("ep", g.at(dz, 0), hid_all.at[me], hid_all.at[me], i1, dz - 1)
        for dz in spread(g.nz)
    }
    i_second = [
        push("ep", g.at(0, dx), hid_all.at[me], hid_all.at[me], i2, dx - 1)
        for dx in range(1, g.nx)
    ]
    for dz in reversed(spread(g.nz)):
        i_first[dz].wait_recv()
        src = g.source(dz, g.nx)
        for dx in range(1, g.nx):
            i_second.append(
                push("ep", g.at(0, dx), hid_all.at[src], hid_all.at[src], i2,
                     dz * (g.nx - 1) + dx - 1)
            )
    sent += list(i_first.values()) + i_second
    hits = jnp.concatenate(
        [returns(me)]
        + [
            returns(g.source((i + 1) // g.nx, (i + 1) % g.nx))
            for i in range(n - 1)
        ],
        axis=1,
    )
    for i in range(n - 1):
        r_copies[i].wait_recv()
    moe = jnp.dot(hits, ret_in[...].reshape(n * half, block), preferred_element_type=F32)
    loads[6].wait()
    for copy in i_second:
        copy.wait_recv()
    dense = jnp.dot(
        hid_all[...].reshape(total_rows, hidden), dd[...], preferred_element_type=F32
    )
    part2[...] = (moe + mix_ref[...] * dense).astype(BF16)
    sent += tp_sum(nt, part2, f_in, f_pair, f_cross, f_full, fs, res)
    out_ref[...] = f_full[...]
    for copy in sent:
        copy.wait_send()


def finish_kernel(a_ref, b_ref, c_ref, a_out, b_out, c_out, sem):
    copies = [
        pltpu.make_async_copy(src, dst, sem.at[i])
        for i, (src, dst) in enumerate(((a_ref, a_out), (b_ref, b_out), (c_ref, c_out)))
    ]
    for copy in copies:
        copy.start()
    for copy in copies:
        copy.wait()


def per_device(
    n, nt, stream, norm_gain, w_query, w_key, w_value, break_offset, cache_keys, cache_values,
    lengths, w_output, head_gain, ffn_gain, route_experts, route_weights, expert_gate,
    expert_up, expert_down, dense_gate, dense_up, dense_down, mix_gain,
):
    total_rows, block = stream.shape
    width = block * n
    rows = lengths.shape[0]
    kv = cache_keys.shape[2]
    hd = cache_keys.shape[3]
    heads = break_offset.shape[0]
    cache_len = cache_keys.shape[1]
    top = route_experts.shape[1]
    hidden = dense_gate.shape[1]
    expert_hidden = expert_gate.shape[2]
    experts = expert_gate.shape[0] * n
    cap = 2 * rows * top // expert_gate.shape[0]
    assert experts == n
    assert nt % 2 == 0 and cap % 2 == 0
    vmem = pl.BlockSpec(memory_space=pltpu.VMEM)
    hbm = pl.BlockSpec(memory_space=pltpu.HBM)
    dma = pltpu.SemaphoreType.DMA
    vm = pltpu.VMEM
    nz, nx = plan(n)
    per = 2
    flat = kv * cache_len
    pairs = rows // per
    m = per * heads
    blocks = flat // 128
    wide = w_query.shape[1] + w_key.shape[1] + w_value.shape[1]
    dt = w_output.shape[0]
    half_cap = (n, cap // 2, block)
    half_rows = (total_rows // 2, block)
    counts = (
        nz * (nx - 1), nz - 1, n - 1, n - 1, n - 1, n - 1, n - 1, nz * (nx - 1), nz - 1,
        nz - 1, nz * (nx - 1), n - 1, nt // 2 + 1, nt // 2 + 1, 1,
    )
    sems = []
    for count in counts:
        sems += [dma((count,)), dma((count,))]
    operands = (
        stream, norm_gain.reshape(1, block), w_query, w_key, w_value, lengths, break_offset,
        head_gain.reshape(heads, hd), ffn_gain.reshape(1, block), mix_gain.reshape(1, block),
        route_experts.T, route_weights.T,
        cache_keys.reshape(rows, flat, hd), cache_values.reshape(rows, flat, hd),
        w_output, dense_gate, dense_up, dense_down, expert_gate, expert_up, expert_down,
    )
    operands = [pltpu.with_memory_space_constraint(a, pltpu.HBM) for a in operands]
    arrays = pl.pallas_call(
        functools.partial(layer_kernel, n, nt, kv, per, width, cap),
        out_shape=(
            jax.ShapeDtypeStruct((total_rows, block), BF16),
            jax.ShapeDtypeStruct((rows, w_key.shape[1]), BF16),
            jax.ShapeDtypeStruct((rows, w_value.shape[1]), BF16),
        ),
        in_specs=[hbm] * 21,
        out_specs=(vmem, vmem, vmem),
        scratch_shapes=[
            vm(stream.shape, BF16),
            vm((1, block), F32),
            vm(w_query.shape, BF16),
            vm(w_key.shape, BF16),
            vm(w_value.shape, BF16),
            pltpu.SMEM((rows,), jnp.int32),
            pltpu.SMEM((heads,), F32),
            vm((heads, hd), F32),
            vm((1, block), F32),
            vm((1, block), F32),
            vm((top, total_rows), jnp.int32),
            vm((top, total_rows), F32),
            dma((12,)),
            vm((rows, flat, hd), BF16),
            vm((rows, flat, hd), BF16),
            vm(w_output.shape, BF16),
            vm(dense_gate.shape, BF16),
            vm(dense_up.shape, BF16),
            vm(dense_down.shape, BF16),
            vm(expert_gate.shape[1:], BF16),
            vm(expert_up.shape[1:], BF16),
            vm(expert_down.shape[1:], BF16),
            dma((pairs,)),
            dma((pairs,)),
            dma((7,)),
            vm((n, rows, wide), BF16),
            vm((nz * (nx - 1), rows, wide), BF16),
            vm((nz - 1, rows, wide), BF16),
            vm((nz - 1, rows, wide), BF16),
            vm((8, total_rows), F32),
            vm((n - 1, 1, total_rows), F32),
            vm((heads, rows, hd), F32),
            vm((pairs, m, flat), F32),
            vm((pairs, m, flat), F32),
            vm((pairs, blocks * m, 256), BF16),
            vm((pairs, blocks * m, 256), F32),
            vm((heads, rows, hd), F32),
            vm((n, rows, dt), BF16),
            vm((total_rows, block), BF16),
            vm((total_rows, block), BF16),
            vm((n - 1, cap // 2, block), BF16),
            vm((n - 1, cap, block), BF16),
            vm((8, total_rows), F32),
            vm((n - 1, 1, total_rows), F32),
            vm((n, rows, 2 * hidden), BF16),
            vm((nz * (nx - 1), rows, 2 * hidden), BF16),
            vm((nz - 1, rows, 2 * hidden), BF16),
            vm((nz - 1, rows, 2 * hidden), BF16),
            vm((n, rows, hidden), BF16),
            vm((cap, expert_hidden), BF16),
            vm((cap, 128), F32),
            vm(half_cap, BF16),
            vm(half_cap, BF16),
            vm(half_cap, F32),
            vm(half_cap, BF16),
            vm((total_rows, block), F32),
        ]
        + [
            vm(half_rows, BF16),
            vm(half_rows, BF16),
            vm((nt // 2 - 1,) + half_rows, BF16),
            vm((total_rows, block), BF16),
        ] * 2
        + sems,
        compiler_params=pltpu.CompilerParams(
            collective_id=0, has_side_effects=True, vmem_limit_bytes=LIMIT_MIB * 1024 * 1024
        ),
        name="layer",
    )(*operands)
    arrays = [pltpu.with_memory_space_constraint(a, pltpu.VMEM) for a in arrays]
    return pl.pallas_call(
        finish_kernel,
        out_shape=tuple(jax.ShapeDtypeStruct(a.shape, a.dtype) for a in arrays),
        in_specs=[vmem] * 3,
        out_specs=(pl.BlockSpec(memory_space=pl.ANY),) * 3,
        scratch_shapes=[dma((3,))],
        name="finish",
    )(*arrays)


def solution(mesh):
    in_specs = (
        P(None, "ep"),
        P("ep"),
        P("ep", "tp"),
        P("ep", "tp"),
        P("ep", "tp"),
        P("tp"),
        P("ep", None, "tp", None),
        P("ep", None, "tp", None),
        P("ep"),
        P("tp", "ep"),
        P("tp"),
        P("ep"),
        P(),
        P(),
        P("ep", None, "tp"),
        P("ep", None, "tp"),
        P("ep", "tp", None),
        P("ep", "tp"),
        P("ep", "tp"),
        P("tp", "ep"),
        P("ep"),
    )
    out_specs = (P(None, "ep"), P("ep", "tp"), P("ep", "tp"))
    body = functools.partial(per_device, mesh.shape["ep"], mesh.shape["tp"])
    return jax.shard_map(
        body, mesh=mesh, in_specs=in_specs, out_specs=out_specs, check_vma=False
    )
```

```python
import functools

import jax
import jax.numpy as jnp
from jax import lax
from jax.experimental import pallas as pl
from jax.experimental.pallas import tpu as pltpu
from jax.sharding import PartitionSpec as P

EPSILON = 1e-06
MESH = pl.DeviceIdType.MESH
F32 = jnp.float32
BF16 = jnp.bfloat16
LIMIT_MIB = 48
NT = (((1,), (1,)), ((), ()))


def row_sums(squares):
    ones = jnp.ones((8, squares.shape[1]), BF16)
    high = squares.astype(BF16)
    low = (squares - high.astype(F32)).astype(BF16)
    return lax.dot_general(ones, high, NT, preferred_element_type=F32) + lax.dot_general(
        ones, low, NT, preferred_element_type=F32
    )


def own_column(sums, first, rows):
    width = sums.shape[1]
    lane = lax.broadcasted_iota(jnp.int32, (rows, width), 1)
    row = lax.broadcasted_iota(jnp.int32, (rows, width), 0)
    return jnp.sum(jnp.where(lane == row + first, sums[0:1, :], 0.0), axis=1, keepdims=True)


def plan(n):
    inner = 1 << ((n.bit_length() - 1) // 2)
    return n // inner, inner


def spread(count):
    return sorted(range(1, count), key=lambda d: abs(2 * d - count))


class Grid:
    def __init__(self, n):
        self.nz, self.nx = plan(n)
        self.me = lax.axis_index("ep")
        self.z = self.me // self.nx
        self.x = lax.rem(self.me, self.nx)

    def at(self, dz, dx):
        return lax.rem(self.z + dz, self.nz) * self.nx + lax.rem(self.x + dx, self.nx)

    def source(self, dz, dx):
        return self.at(self.nz - dz, self.nx - dx)

    def peers(self):
        order = spread(self.nz)
        return [(dz, dx) for dz in order for dx in range(self.nx)] + [
            (0, dx) for dx in range(1, self.nx)
        ]


def signal_all(axes):
    barrier = pltpu.get_barrier_semaphore()
    total = 0
    for axis, count in axes:
        me = lax.axis_index(axis)
        for k in range(1, count):
            pl.semaphore_signal(
                barrier, inc=1, device_id={axis: lax.rem(me + k, count)}, device_id_type=MESH
            )
            total += 1
    return barrier, total


def push(axis, peer, src, dst, sems, i):
    copy = pltpu.make_async_remote_copy(
        src_ref=src,
        dst_ref=dst,
        send_sem=sems[0].at[i if sems[0].shape[0] > 1 else 0],
        recv_sem=sems[1].at[i if sems[1].shape[0] > 1 else 0],
        device_id={axis: peer},
        device_id_type=MESH,
    )
    copy.start()
    return copy


def drain(ref, sems):
    pltpu.make_async_copy(ref, ref, sems.at[0]).wait()


def scatter_first(g, part, got, sems):
    copies = {}
    for dz in spread(g.nz) + [0]:
        for dx in range(1, g.nx):
            i = dz * (g.nx - 1) + dx - 1
            copies[dz, dx] = push("ep", g.at(0, dx), part.at[g.at(dz, dx)], got.at[i], sems, i)
    return copies


def scatter_next(g, part, got, copies, mid, got2, sems, dz):
    acc = part[g.at(dz, 0)].astype(F32)
    for dx in range(1, g.nx):
        copies[dz, dx].wait_recv()
        acc = acc + got[dz * (g.nx - 1) + dx - 1].astype(F32)
    if dz == 0:
        return acc
    mid[dz - 1] = acc.astype(BF16)
    return push("ep", g.at(dz, 0), mid.at[dz - 1], got2.at[dz - 1], sems, dz - 1)


def tp_sum(nt, part, arrived, pair, crossed, full, sems, extra):
    me = lax.axis_index("tp")
    core = lax.rem(me, 2)
    partner = me + 1 - 2 * core
    half = pair.shape[0]
    mine = pl.ds(pl.multiple_of(core * half, half), half)
    other = pl.ds(pl.multiple_of((1 - core) * half, half), half)
    copies = [push("tp", partner, part.at[other], arrived, sems, 0)]
    copies[0].wait_recv()
    pair[...] = (part[mine].astype(F32) + arrived[...].astype(F32)).astype(BF16)
    for j in range(1, nt // 2):
        copies.append(push("tp", lax.rem(me + 2 * j, nt), pair, crossed.at[j - 1], sems, j))
    total = pair[...].astype(F32)
    for j in range(1, nt // 2):
        copies[j].wait_recv()
        total = total + crossed[j - 1].astype(F32)
    if extra is not None:
        total = total + extra[mine]
    full[mine] = total.astype(BF16)
    copies.append(push("tp", partner, full.at[mine], full.at[mine], sems, nt // 2))
    copies[-1].wait_recv()
    return copies


def attend(kv, per, waits, len_ref, off_ref, gain_ref, q_s, k_s, v_s, sc_s, sg_s, hl_s, sm_s,
           ho_s):
    heads, rows, hd = q_s.shape
    cols = k_s.shape[1]
    group = heads // kv
    m = per * heads
    lanes = 128
    blocks = cols // lanes
    pairs = rows // per
    row_q = lax.broadcasted_iota(jnp.int32, (m, hd), 0)
    row = lax.broadcasted_iota(jnp.int32, (m, lanes), 0)
    lane = lax.broadcasted_iota(jnp.int32, (m, lanes), 1)
    for load in waits[0]:
        load.wait()
    for p in range(pairs):
        q = jnp.concatenate(
            [q_s[h, pl.ds(p * per + s, 1), :] for s in range(per) for h in range(heads)], axis=0
        )
        wide = jnp.concatenate(
            [jnp.where(row_q // heads == s, q, 0.0) for s in range(per)], axis=1
        ).astype(BF16)
        keys = jnp.concatenate([k_s[p * per + s] for s in range(per)], axis=1)
        sc_s[p] = lax.dot_general(wide, keys, NT, preferred_element_type=F32)
    offset = jnp.zeros((m, lanes), F32)
    for h in range(heads):
        offset = jnp.where(row % heads == h, off_ref[h], offset)
    mine = (row % heads) // group == lane % kv
    limits = []
    for p in range(pairs):
        length = jnp.zeros((m, lanes), jnp.int32)
        for s in range(per):
            length = jnp.where(row // heads == s, len_ref[p * per + s], length)
        limit = jnp.where(mine, length * kv - lane, -cols)
        limits.append(limit)
        fails = []
        for b in range(blocks):
            sc = sc_s[p, :, b * lanes : (b + 1) * lanes] * hd ** (-0.5) + offset
            ls = jnp.minimum(sc, 0.0) - jnp.log(1.0 + jnp.exp(-jnp.abs(sc)))
            sg_s[p, :, b * lanes : (b + 1) * lanes] = ls
            fails.append(jnp.where(limit > b * lanes, ls - sc, 0.0))
        failed = jnp.concatenate(fails, axis=0)
        high = failed.astype(BF16)
        low = (failed - high.astype(F32)).astype(BF16)
        hl_s[p] = jnp.concatenate([high, low], axis=1)
    r = lax.broadcasted_iota(jnp.int32, (2 * lanes, 2 * lanes), 0) % lanes
    c = lax.broadcasted_iota(jnp.int32, (2 * lanes, 2 * lanes), 1)
    tri = jnp.where((r > c) | (c >= lanes), 1.0, 0.0).astype(BF16)
    for p in range(pairs):
        sm_s[p] = jnp.dot(hl_s[p], tri, preferred_element_type=F32)
    gains = jnp.concatenate([gain_ref[...]] * per, axis=0)
    for load in waits[1]:
        load.wait()
    for p in range(pairs):
        acc = jnp.zeros((m, lanes), F32)
        weights = [None] * blocks
        for b in reversed(range(blocks)):
            later = sm_s[p, b * m : (b + 1) * m, :lanes] + acc
            acc = acc + sm_s[p, b * m : (b + 1) * m, lanes:]
            weights[b] = jnp.where(
                limits[p] > b * lanes,
                jnp.exp(sg_s[p, :, b * lanes : (b + 1) * lanes] + later),
                0.0,
            )
        weights = jnp.concatenate(weights, axis=1).astype(BF16)
        values = jnp.concatenate([v_s[p * per + s] for s in range(per)], axis=1)
        both = jnp.dot(weights, values, preferred_element_type=F32)
        att = both[:, :hd]
        for s in range(1, per):
            att = jnp.where(row_q // heads == s, both[:, s * hd : (s + 1) * hd], att)
        att = att * lax.rsqrt(jnp.mean(att * att, axis=1, keepdims=True) + EPSILON) * gains
        for s in range(per):
            for h in range(heads):
                ho_s[h, pl.ds(p * per + s, 1), :] = att[s * heads + h : s * heads + h + 1]


def layer_kernel(
    n, nt, kv, per, width, cap,
    x_hbm, g_hbm, wq_hbm, wk_hbm, wv_hbm,
    len_hbm, off_hbm, gain_hbm, fg_hbm, mix_hbm, route_hbm, route_w_hbm,
    key_hbm, val_hbm, wo_hbm, dg_hbm, du_hbm, dd_hbm, eg_hbm, eu_hbm, ed_hbm,
    out_ref, k_ref, v_ref,
    x_ref, g_ref, wq_ref, wk_ref, wv_ref,
    len_ref, off_ref, gain_ref, fg_ref, mix_ref, route_ref, route_w_ref, e_sem,
    k_s, v_s, wo, dg, du, dd, eg, eu, ed, k_sem, v_sem, w_sem,
    p_part, p_got, p_mid, p_got2, t_part, t_got, t_mid, t_got2, p_sums, p_sums_in,
    q_s, sc_s, sg_s, hl_s, sm_s, ho_s,
    heads_all, part, part2, disp, disp_in, sums, sums_in,
    gu, gu_got, gu_mid, gu_got2, hid_all,
    ret_x, ret_p, ret_m, ret_o, ret_y, ret_b, ret, ret_in, res,
    a_in, a_pair, a_cross, a_full, f_in, f_pair, f_cross, f_full,
    *sem_refs,
):
    (p1, p2, t1, t2, ps, hs, ds, ws, ys, ss, g1, g2, i1, i2, rs, as_, fs, xs, bs) = [
        (sem_refs[2 * i], sem_refs[2 * i + 1]) for i in range(len(sem_refs) // 2)
    ]
    g = Grid(n)
    me = g.me
    barrier, greetings = signal_all((("ep", n), ("tp", nt)))
    early = [
        pltpu.make_async_copy(src, dst, e_sem.at[i])
        for i, (src, dst) in enumerate(
            ((x_hbm, x_ref), (g_hbm, g_ref), (wq_hbm, wq_ref), (wk_hbm, wk_ref),
             (wv_hbm, wv_ref), (len_hbm, len_ref), (off_hbm, off_ref), (gain_hbm, gain_ref),
             (fg_hbm, fg_ref), (mix_hbm, mix_ref), (route_hbm, route_ref),
             (route_w_hbm, route_w_ref))
        )
    ]
    for load in early:
        load.start()
    chunk = k_s.shape[0] // 2
    k_loads, v_loads = [], []
    for p in range(2):
        rng = pl.ds(p * chunk, chunk)
        k_loads.append(pltpu.make_async_copy(key_hbm.at[rng], k_s.at[rng], k_sem.at[p]))
        v_loads.append(pltpu.make_async_copy(val_hbm.at[rng], v_s.at[rng], v_sem.at[p]))
    loads = [
        pltpu.make_async_copy(src, dst, w_sem.at[i])
        for i, (src, dst) in enumerate(
            ((wo_hbm, wo), (dg_hbm, dg), (du_hbm, du), (eg_hbm.at[0], eg), (eu_hbm.at[0], eu),
             (ed_hbm.at[0], ed), (dd_hbm, dd))
        )
    ]
    total_rows, block = x_ref.shape
    rows = total_rows // n
    sent = []

    for load in early:
        load.wait()
    for load in k_loads + v_loads + loads:
        load.start()
    x = x_ref[...].astype(F32)
    xg = (x * g_ref[...]).astype(BF16)
    p_sums[...] = row_sums(x * x)
    at = 0
    for w_ref, dest in ((wq_ref, p_part), (wk_ref, t_part), (wv_ref, t_part)):
        cols = w_ref.shape[1]
        at = wk_ref.shape[1] if w_ref is wv_ref else 0
        val = jnp.dot(xg, w_ref[...], preferred_element_type=F32).astype(BF16)
        for i in range(n):
            dest[i, :, at : at + cols] = val[i * rows : (i + 1) * rows]
    pl.semaphore_wait(barrier, greetings)
    first = scatter_first(g, p_part, p_got, p1)
    for dz, dx in g.peers():
        i = dz * g.nx + dx - 1
        push("ep", g.at(dz, dx), p_sums.at[pl.ds(0, 1)], p_sums_in.at[i], ps, i)
    t_first = scatter_first(g, t_part, t_got, t1)
    second = {}
    for dz in spread(g.nz) + [0]:
        second[dz] = scatter_next(g, p_part, p_got, first, p_mid, p_got2, p2, dz)
    total = second.pop(0)
    drain(p_sums_in, ps[1])
    squares = p_sums[0:1, :]
    for i in range(n - 1):
        squares = squares + p_sums_in[i]
    inverse = lax.rsqrt(own_column(squares, me * rows, rows) / width + EPSILON)
    for dz in second:
        second[dz].wait_recv()
        total = total + p_got2[dz - 1].astype(F32)
    total = total * inverse
    hd = q_s.shape[2]
    for h in range(q_s.shape[0]):
        q_s[h] = total[:, h * hd : (h + 1) * hd].astype(BF16).astype(F32)
    t_second = {}
    for dz in spread(g.nz) + [0]:
        t_second[dz] = scatter_next(g, t_part, t_got, t_first, t_mid, t_got2, t2, dz)
    rows_kv = t_second.pop(0)

    attend(kv, per, (k_loads, v_loads), len_ref, off_ref, gain_ref, q_s, k_s, v_s, sc_s, sg_s,
           hl_s, sm_s, ho_s)
    heads_all[me] = jnp.concatenate(
        [ho_s[h] for h in range(ho_s.shape[0])], axis=1
    ).astype(BF16)
    for dz, dx in g.peers():
        push("ep", g.at(dz, dx), heads_all.at[me], heads_all.at[me], hs, dz * g.nx + dx - 1)
    for dz in t_second:
        t_second[dz].wait_recv()
        rows_kv = rows_kv + t_got2[dz - 1].astype(F32)
    rows_kv = rows_kv * inverse
    k_ref[...] = rows_kv[:, : k_ref.shape[1]].astype(BF16)
    v_ref[...] = rows_kv[:, k_ref.shape[1] :].astype(BF16)
    me_t = lax.axis_index("tp")
    core = lax.rem(me_t, 2)
    partner = me_t + 1 - 2 * core
    lines = nt // 2
    part_cap = cap // nt
    me_y = me_t // 2
    top = route_ref.shape[0]
    expert_ids = lax.broadcasted_iota(jnp.int32, (n, total_rows), 0)
    named = [
        jnp.where(route_ref[k : k + 1, :] == expert_ids, 1.0, 0.0).astype(F32)
        for k in range(top)
    ]
    token_r = lax.broadcasted_iota(jnp.int32, (total_rows, total_rows), 0)
    token_c = lax.broadcasted_iota(jnp.int32, (total_rows, total_rows), 1)
    before = jnp.dot(
        sum(named).astype(BF16),
        jnp.where(token_r < token_c, 1.0, 0.0).astype(BF16),
        preferred_element_type=F32,
    )
    slots = [
        jnp.sum(named[k] * before, axis=0, keepdims=True)
        + route_ref[k : k + 1, :].astype(F32) * cap
        for k in range(top)
    ]
    columns = [
        jnp.sum(jnp.where(token_r == token_c, slot, 0.0), axis=1, keepdims=True)
        for slot in slots
    ]
    share_sum = route_w_ref[0:1, :]
    for k in range(1, top):
        share_sum = share_sum + route_w_ref[k : k + 1, :]
    share_rows = [route_w_ref[k : k + 1, :] / share_sum for k in range(top)]
    def slot_of(place):
        spot = place // part_cap
        line = lax.rem(me_y + spot % lines, lines)
        lane_core = jnp.where(spot < lines, 1 - core, core)
        return (line * 2 + lane_core) * part_cap + place % part_cap

    slot_rows = slot_of(lax.broadcasted_iota(jnp.int32, (cap, total_rows), 0))
    own_rows = lax.broadcasted_iota(jnp.int32, (part_cap, total_rows), 0) + me_t * part_cap

    def picks(expert, places):
        place = (places + expert * cap).astype(F32)
        return [slot == place for slot in slots]

    peers = g.peers()
    mine = picks(me, slot_rows)
    hit = functools.reduce(jnp.logical_or, mine)
    chosen = jnp.concatenate(
        [
            jnp.where(functools.reduce(jnp.logical_or, picks(g.at(dz, dx), own_rows)), 1.0, 0.0)
            for dz, dx in peers
        ]
        + [jnp.where(hit, 1.0, 0.0)],
        axis=0,
    ).astype(BF16)
    slot_cols = lax.broadcasted_iota(jnp.int32, (total_rows, n * part_cap), 1)
    source = slot_cols // part_cap
    source = lax.rem(me // g.nx + g.nz - source // g.nx, g.nz) * g.nx + lax.rem(
        lax.rem(me, g.nx) + g.nx - source % g.nx, g.nx
    )
    slot_cols = (source * cap + me_t * part_cap + slot_cols % part_cap).astype(F32)
    hits = jnp.where(
        functools.reduce(jnp.logical_or, [column == slot_cols for column in columns]), 1.0, 0.0
    ).astype(BF16)

    loads[0].wait()
    drain(heads_all.at[pl.ds(0, n - 1)], hs[1])
    all_heads = heads_all[...].reshape(total_rows, heads_all.shape[2])
    part[...] = jnp.dot(all_heads, wo[...], preferred_element_type=F32).astype(BF16)
    sent += tp_sum(nt, part, a_in, a_pair, a_cross, a_full, as_, None)
    residual = x_ref[...].astype(F32) + a_full[...].astype(F32)
    u = (residual * fg_ref[...]).astype(BF16)
    sums[...] = row_sums(residual * residual)
    res[...] = residual
    packed = jnp.dot(chosen, u, preferred_element_type=F32).astype(BF16)
    d_copies = {}
    for j, (dz, dx) in enumerate(peers):
        i = dz * g.nx + dx - 1
        disp[i] = packed[j * part_cap : (j + 1) * part_cap]
        d_copies[i] = push("ep", g.at(dz, dx), disp.at[i], disp_in.at[i, lines], ds, i)
    for dz, dx in peers:
        i = dz * g.nx + dx - 1
        push("ep", g.at(dz, dx), sums.at[pl.ds(0, 1)], sums_in.at[i], ss, i)
    own_in = packed[len(peers) * part_cap :]
    hidden = dg.shape[1]
    for load, w, at in ((loads[1], dg, 0), (loads[2], du, hidden)):
        load.wait()
        val = jnp.dot(u, w[...], preferred_element_type=F32).astype(BF16)
        for i in range(n):
            gu[i, :, at : at + hidden] = val[i * rows : (i + 1) * rows]
    g_first = scatter_first(g, gu, gu_got, g1)
    loads[3].wait()
    loads[4].wait()
    span = pl.ds(pl.multiple_of(me * block, block), block)
    gate = jnp.dot(own_in, eg[span, :], preferred_element_type=F32)
    up = jnp.dot(own_in, eu[span, :], preferred_element_type=F32)
    squares = sums[0:1, :]
    order = list(reversed(peers))
    g_order = spread(g.nz) + [0]
    g_second = {}
    y_copies, c_copies = {}, {}

    def arrive(i):
        d_copies[i].wait_recv()
        at = disp_in.at[i, lines]
        c_copies[i, 0] = push("tp", partner, at, disp_in.at[i, 0], ws, i * lines)
        for k in range(1, lines):
            y_copies[i, k] = push(
                "tp", lax.rem(me_t + 2 * k, nt), at, disp_in.at[i, 2 * lines - k], ys,
                i * (lines - 1) + k - 1,
            )

    def relay(i):
        for k in range(1, lines):
            y_copies[i, k].wait_recv()
            at = disp_in.at[i, 2 * lines - k]
            c_copies[i, lines - k] = push(
                "tp", partner, at, disp_in.at[i, lines - k], ws, i * lines + lines - k
            )

    def regroup():
        dz = g_order[len(g_second)]
        g_second[dz] = scatter_next(g, gu, gu_got, g_first, gu_mid, gu_got2, g2, dz)

    def consume(j):
        dz, dx = order[j]
        i = index[j]
        for k in range(lines):
            c_copies[i, k].wait_recv()
        span = pl.ds(pl.multiple_of(g.source(dz, dx) * block, block), block)
        rows_in = disp_in[i].reshape(cap, block)
        return (
            gate + jnp.dot(rows_in, eg[span, :], preferred_element_type=F32),
            up + jnp.dot(rows_in, eu[span, :], preferred_element_type=F32),
        )

    index = [dz * g.nx + dx - 1 for dz, dx in order]
    count = len(index)
    for i in index:
        arrive(i)
    stops = [0, count // 2 + 1]
    for j, i in enumerate(index):
        if j in stops:
            regroup()
        relay(i)
    drain(sums_in, ss[1])
    for i in range(n - 1):
        squares = squares + sums_in[i]
    for j in range(count):
        if j == count // 2 and len(g_second) < len(g_order) - 1:
            regroup()
        gate, up = consume(j)
    scale_row = lax.rsqrt(squares / width + EPSILON)
    scale = jnp.sum(jnp.where(hit, scale_row, 0.0), axis=1, keepdims=True)
    share = jnp.zeros((cap, 1), F32)
    for k in range(len(mine)):
        share = share + jnp.sum(
            jnp.where(mine[k], share_rows[k], 0.0), axis=1, keepdims=True
        )
    gate = gate * scale
    up = up * scale
    act = (gate / (1.0 + jnp.exp(-gate)) * up).astype(BF16)
    loads[5].wait()
    dests = peers + [(0, 0)]
    swaps, backs, r_copies = [], {}, {}
    out = jnp.dot(act, ed[...], preferred_element_type=F32) * share
    for i in range(n):
        ret_x[i] = out[: cap // 2, i * block : (i + 1) * block].astype(BF16)
        ret_m[i] = out[cap // 2 :, i * block : (i + 1) * block]
    for j, (dz, dx) in enumerate(dests):
        swaps.append(push("tp", partner, ret_x.at[g.at(dz, dx)], ret_p.at[j], xs, j))
    while len(g_second) < len(g_order):
        regroup()
    gate_up = g_second.pop(0)
    for j, (dz, dx) in enumerate(dests):
        swaps[j].wait_recv()
        out = ret_m[g.at(dz, dx)] + ret_p[j].astype(F32)
        ret_o[j] = out[:part_cap]
        for k in range(1, lines):
            ret_y[j, k - 1] = out[k * part_cap : (k + 1) * part_cap].astype(BF16)
            backs[j, k] = push(
                "tp", lax.rem(me_t + 2 * k, nt), ret_y.at[j, k - 1], ret_b.at[j, k - 1], bs,
                j * (lines - 1) + k - 1,
            )
    for dz in g_second:
        g_second[dz].wait_recv()
        gate_up = gate_up + gu_got2[dz - 1].astype(F32)
    gate_up = gate_up * own_column(scale_row, me * rows, rows)
    dense_gate = gate_up[:, :hidden]
    hid_all[me] = (dense_gate / (1.0 + jnp.exp(-dense_gate)) * gate_up[:, hidden:]).astype(BF16)
    i_first = {
        dz: push("ep", g.at(dz, 0), hid_all.at[me], hid_all.at[me], i1, dz - 1)
        for dz in spread(g.nz)
    }
    for dx in range(1, g.nx):
        push("ep", g.at(0, dx), hid_all.at[me], hid_all.at[me], i2, dx - 1)
    pending = list(reversed(spread(g.nz)))

    def spread_hidden():
        dz = pending.pop(0)
        i_first[dz].wait_recv()
        src = g.source(dz, g.nx)
        for dx in range(1, g.nx):
            push("ep", g.at(0, dx), hid_all.at[src], hid_all.at[src], i2,
                 dz * (g.nx - 1) + dx - 1)

    for j, (dz, dx) in enumerate(dests):
        out = ret_o[j]
        for k in range(1, lines):
            backs[j, k].wait_recv()
            out = out + ret_b[j, k - 1].astype(F32)
        i = dz * g.nx + dx
        if i == 0:
            ret_in[0] = out.astype(BF16)
        else:
            ret[j] = out.astype(BF16)
            r_copies[i] = push("ep", g.at(dz, dx), ret.at[j], ret_in.at[i], rs, i - 1)
        if pending and n - j <= len(pending) + 1:
            spread_hidden()
    while pending:
        spread_hidden()
    loads[6].wait()
    drain(hid_all.at[pl.ds(0, g.nz * (g.nx - 1))], i2[1])
    dense = jnp.dot(
        hid_all[...].reshape(total_rows, hidden), dd[...], preferred_element_type=F32
    )
    drain(ret_in.at[pl.ds(1, n - 1)], rs[1])
    moe = jnp.dot(hits, ret_in[...].reshape(n * part_cap, block), preferred_element_type=F32)
    part2[...] = (moe + mix_ref[...] * dense).astype(BF16)
    sent += tp_sum(nt, part2, f_in, f_pair, f_cross, f_full, fs, res)
    out_ref[...] = f_full[...]
    for copy in sent:
        copy.wait_send()
    for sems, ref in (
        (p1, p_got), (p2, p_mid), (t1, t_got), (t2, t_mid), (ps, p_sums_in),
        (hs, heads_all.at[pl.ds(0, n - 1)]), (ds, disp), (ws, disp_in.at[:, pl.ds(0, lines)]),
        (ys, ret_y.at[pl.ds(0, n - 1)]), (ss, sums_in), (g1, gu_got), (g2, gu_mid),
        (i1, hid_all.at[pl.ds(0, g.nz - 1)]), (i2, hid_all.at[pl.ds(0, g.nz * (g.nx - 1))]),
        (rs, ret.at[pl.ds(0, n - 1)]), (xs, ret_x), (bs, ret_y),
    ):
        drain(ref, sems[0])


def finish_kernel(a_ref, b_ref, c_ref, a_out, b_out, c_out, sem):
    copies = [
        pltpu.make_async_copy(src, dst, sem.at[i])
        for i, (src, dst) in enumerate(((a_ref, a_out), (b_ref, b_out), (c_ref, c_out)))
    ]
    for copy in copies:
        copy.start()
    for copy in copies:
        copy.wait()


def per_device(
    n, nt, stream, norm_gain, w_query, w_key, w_value, break_offset, cache_keys, cache_values,
    lengths, w_output, head_gain, ffn_gain, route_experts, route_weights, expert_gate,
    expert_up, expert_down, dense_gate, dense_up, dense_down, mix_gain,
):
    total_rows, block = stream.shape
    width = block * n
    rows = lengths.shape[0]
    kv = cache_keys.shape[2]
    hd = cache_keys.shape[3]
    heads = break_offset.shape[0]
    cache_len = cache_keys.shape[1]
    top = route_experts.shape[1]
    hidden = dense_gate.shape[1]
    experts = expert_gate.shape[0] * n
    cap = 2 * rows * top // expert_gate.shape[0]
    assert experts == n
    assert nt % 2 == 0 and cap % nt == 0
    vmem = pl.BlockSpec(memory_space=pltpu.VMEM)
    hbm = pl.BlockSpec(memory_space=pltpu.HBM)
    dma = pltpu.SemaphoreType.DMA
    vm = pltpu.VMEM
    nz, nx = plan(n)
    per = 2
    flat = kv * cache_len
    pairs = rows // per
    m = per * heads
    blocks = flat // 128
    dt = w_output.shape[0]
    lines = nt // 2
    part_cap = cap // nt
    half_rows = (total_rows // 2, block)
    first, second, relays = nz * (nx - 1), nz - 1, (n - 1) * lines
    counts = (
        (1, first), (1, second), (1, first), (1, second), (1, 1), (1, 1), (1, n - 1),
        (1, relays), (1, relays - n + 1), (1, 1), (1, first), (1, second), (1, second), (1, 1),
        (1, 1), (lines + 1,) * 2, (lines + 1,) * 2, (1, n), (1, n * (lines - 1)),
    )
    sems = [dma((count,)) for pair in counts for count in pair]
    operands = (
        stream, norm_gain.reshape(1, block), w_query, w_key, w_value, lengths, break_offset,
        head_gain.reshape(heads, hd), ffn_gain.reshape(1, block), mix_gain.reshape(1, block),
        route_experts.T, route_weights.T,
        cache_keys.reshape(rows, flat, hd), cache_values.reshape(rows, flat, hd),
        w_output, dense_gate, dense_up, dense_down, expert_gate, expert_up, expert_down,
    )
    operands = [pltpu.with_memory_space_constraint(a, pltpu.HBM) for a in operands]
    arrays = pl.pallas_call(
        functools.partial(layer_kernel, n, nt, kv, per, width, cap),
        out_shape=(
            jax.ShapeDtypeStruct((total_rows, block), BF16),
            jax.ShapeDtypeStruct((rows, w_key.shape[1]), BF16),
            jax.ShapeDtypeStruct((rows, w_value.shape[1]), BF16),
        ),
        in_specs=[hbm] * 21,
        out_specs=(vmem, vmem, vmem),
        scratch_shapes=[
            vm(stream.shape, BF16),
            vm((1, block), F32),
            vm(w_query.shape, BF16),
            vm(w_key.shape, BF16),
            vm(w_value.shape, BF16),
            pltpu.SMEM((rows,), jnp.int32),
            pltpu.SMEM((heads,), F32),
            vm((heads, hd), F32),
            vm((1, block), F32),
            vm((1, block), F32),
            vm((top, total_rows), jnp.int32),
            vm((top, total_rows), F32),
            dma((12,)),
            vm((rows, flat, hd), BF16),
            vm((rows, flat, hd), BF16),
            vm(w_output.shape, BF16),
            vm(dense_gate.shape, BF16),
            vm(dense_up.shape, BF16),
            vm(dense_down.shape, BF16),
            vm(expert_gate.shape[1:], BF16),
            vm(expert_up.shape[1:], BF16),
            vm(expert_down.shape[1:], BF16),
            dma((2,)),
            dma((2,)),
            dma((7,)),
        ]
        + [
            vm((count, rows, cols), BF16)
            for cols in (w_query.shape[1], w_key.shape[1] + w_value.shape[1])
            for count in (n, nz * (nx - 1), nz - 1, nz - 1)
        ]
        + [
            vm((8, total_rows), F32),
            vm((n - 1, 1, total_rows), F32),
            vm((heads, rows, hd), F32),
            vm((pairs, m, flat), F32),
            vm((pairs, m, flat), F32),
            vm((pairs, blocks * m, 256), BF16),
            vm((pairs, blocks * m, 256), F32),
            vm((heads, rows, hd), F32),
            vm((n, rows, dt), BF16),
            vm((total_rows, block), BF16),
            vm((total_rows, block), BF16),
            vm((n - 1, part_cap, block), BF16),
            vm((n - 1, nt, part_cap, block), BF16),
            vm((8, total_rows), F32),
            vm((n - 1, 1, total_rows), F32),
            vm((n, rows, 2 * hidden), BF16),
            vm((nz * (nx - 1), rows, 2 * hidden), BF16),
            vm((nz - 1, rows, 2 * hidden), BF16),
            vm((nz - 1, rows, 2 * hidden), BF16),
            vm((n, rows, hidden), BF16),
            vm((n, cap // 2, block), BF16),
            vm((n, cap // 2, block), BF16),
            vm((n, cap // 2, block), F32),
            vm((n, part_cap, block), F32),
            vm((n, lines - 1, part_cap, block), BF16),
            vm((n, lines - 1, part_cap, block), BF16),
            vm((n, part_cap, block), BF16),
            vm((n, part_cap, block), BF16),
            vm((total_rows, block), F32),
        ]
        + [
            vm(half_rows, BF16),
            vm(half_rows, BF16),
            vm((nt // 2 - 1,) + half_rows, BF16),
            vm((total_rows, block), BF16),
        ] * 2
        + sems,
        compiler_params=pltpu.CompilerParams(
            collective_id=0, has_side_effects=True, vmem_limit_bytes=LIMIT_MIB * 1024 * 1024
        ),
        name="layer",
    )(*operands)
    arrays = [pltpu.with_memory_space_constraint(a, pltpu.VMEM) for a in arrays]
    return pl.pallas_call(
        finish_kernel,
        out_shape=tuple(jax.ShapeDtypeStruct(a.shape, a.dtype) for a in arrays),
        in_specs=[vmem] * 3,
        out_specs=(pl.BlockSpec(memory_space=pl.ANY),) * 3,
        scratch_shapes=[dma((3,))],
        name="finish",
    )(*arrays)


def solution(mesh):
    in_specs = (
        P(None, "ep"),
        P("ep"),
        P("ep", "tp"),
        P("ep", "tp"),
        P("ep", "tp"),
        P("tp"),
        P("ep", None, "tp", None),
        P("ep", None, "tp", None),
        P("ep"),
        P("tp", "ep"),
        P("tp"),
        P("ep"),
        P(),
        P(),
        P("ep", None, "tp"),
        P("ep", None, "tp"),
        P("ep", "tp", None),
        P("ep", "tp"),
        P("ep", "tp"),
        P("tp", "ep"),
        P("ep"),
    )
    out_specs = (P(None, "ep"), P("ep", "tp"), P("ep", "tp"))
    body = functools.partial(per_device, mesh.shape["ep"], mesh.shape["tp"])
    return jax.shard_map(
        body, mesh=mesh, in_specs=in_specs, out_specs=out_specs, check_vma=False
    )
```
